32 devices in a mesh: ep: 16 (over z, y, x), tp: 2 (over core).
Axes of the slice: x: 2, y: 2, z: 4, core: 2. Of those that a mesh axis runs over, the one named last changes fastest.
Arguments:
- tokens: bfloat16 [256, 2048], P(('ep', 'tp')), may hold values from -6 to 6
- mix_gain: float32 [2048], replicated, may hold values from 0.1 to 1.9
- w_query: bfloat16 [2048, 16, 128], P(None, 'tp', 'ep'), may hold values from -0.125 to 0.125
- w_key: bfloat16 [2048, 16, 128], P(None, 'tp', 'ep'), may hold values from -0.125 to 0.125
- w_value: bfloat16 [2048, 16, 128], P(None, 'tp', 'ep'), may hold values from -0.125 to 0.125
- w_zgate: bfloat16 [2048, 16, 128], P(None, 'tp', 'ep'), may hold values from -0.125 to 0.125
- w_beta: bfloat16 [2048, 16], P(None, 'tp'), may hold values from -0.125 to 0.125
- w_decay: bfloat16 [2048, 16], P(None, 'tp'), may hold values from -0.125 to 0.125
- decay_rate: float32 [16], P('tp'), may hold values from 0.5 to 8
- decay_bias: float32 [16], P('tp'), may hold values from -3 to 0
- head_gain: float32 [128], replicated, may hold values from 0.1 to 1.9
- state: float32 [256, 16, 128, 128], P('ep', 'tp'), may hold values from -1.5 to 1.5
- w_out: bfloat16 [2048, 2048], P('tp', 'ep'), may hold values from -0.125 to 0.125
- moe_gain: float32 [2048], replicated, may hold values from 0.1 to 1.9
- dense_mix: bfloat16 [2048], replicated, may hold values from -0.125 to 0.125
- dense_gate: bfloat16 [2048, 4096], P(None, ('ep', 'tp')), may hold values from -0.125 to 0.125
- dense_up: bfloat16 [2048, 4096], P(None, ('ep', 'tp')), may hold values from -0.125 to 0.125
- dense_down: bfloat16 [4096, 2048], P(('ep', 'tp')), may hold values from -0.09375 to 0.09375
- expert_gate: bfloat16 [16, 2048, 1024], P('ep', None, 'tp'), may hold values from -0.125 to 0.125
- expert_up: bfloat16 [16, 2048, 1024], P('ep', None, 'tp'), may hold values from -0.125 to 0.125
- expert_down: bfloat16 [16, 1024, 2048], P('ep', 'tp'), may hold values from -0.1875 to 0.1875
- expert_ids: int32 [256, 4], replicated, may hold values from 0 to 15, as said below
- route_weight: float32 [256, 4], replicated, may hold values from 0.1 to 1
Outputs:
- layer_out: bfloat16 [256, 2048], P(('ep', 'tp'))
- new_state: float32 [256, 16, 128, 128], P('ep', 'tp')
The draws below stay inside these ranges and needn't reach their ends.
Inputs may be any that keep to these rules, and one draw needn't show every extreme that they name: `expert_ids`: the 4 experts of a row are distinct and lie in one group of 8 consecutive ids. In each aligned block of 16 rows (the rows of one index of ep) no expert is named by more than 8 rows, and at most 16 rows pick one group.
All inputs are finite; a program needn't handle non-finite values.
Results may differ from the reference program's by a relative error of at most 0.012.
Values may be sent and summed in bfloat16 or wider, within the bound.
A program may use at most 128 MiB of HBM per device.

```python
import math
import jax
import jax.numpy as jnp
from jax import lax

D = 2048
HEADS = 16
HEAD = 128
FFE = 1024
FFD = 4096
EPG = 8
TOP_K = 4
SEQ_GROUP = 16
HD = 2048
EXPERTS = 16
GROUPS = 2
GCAP = 16
CAP = 8
SLOTS = 128
TOKENS = 256


def draw_expert_ids(key, part):
    base = jax.random.fold_in(key, 11)
    key_hot, key_blocks = jax.random.split(base)
    hot_base = jax.random.randint(key_hot, (), 0, GROUPS)
    block_count = TOKENS // SEQ_GROUP

    def one_block(block_key, block_number):
        hot_group = (hot_base + block_number) % GROUPS
        key_pool, key_order, key_labels = jax.random.split(block_key, 3)
        others = (hot_group + 1 + jnp.repeat(jnp.arange(GROUPS - 1, dtype=jnp.int32), GCAP)) % GROUPS
        others = jax.random.permutation(key_pool, others)
        pool = jnp.concatenate([jnp.full((GCAP,), hot_group, jnp.int32), others.astype(jnp.int32)])[:SEQ_GROUP]
        groups = jax.random.permutation(key_order, pool)
        positions = jnp.arange(SEQ_GROUP, dtype=jnp.int32)
        same_group = groups[:, None] == groups[None, :]
        earlier = positions[None, :] < positions[:, None]
        rank_in = jnp.sum((same_group & earlier).astype(jnp.int32), axis=1)
        local = (rank_in[:, None] * TOP_K + jnp.arange(TOP_K, dtype=jnp.int32)[None, :]) % EPG
        labels = jax.vmap(lambda label_key: jax.random.permutation(label_key, EPG))(jax.random.split(key_labels, GROUPS)).astype(jnp.int32)
        chosen = labels[groups[:, None], local]
        return (groups[:, None] * EPG + chosen).astype(jnp.int32)
    blocks = jax.vmap(one_block)(jax.random.split(key_blocks, block_count), jnp.arange(block_count, dtype=jnp.int32))
    return blocks.reshape(TOKENS, TOP_K).astype(jnp.int32)


def shard_levels(key, dims, pieces, smallest, largest):
    level = 1.0
    for position, blocks in pieces:
        draws = jax.random.uniform(jax.random.fold_in(jax.random.fold_in(key, 6), position), (blocks,), jnp.float32, smallest / len(pieces), largest / len(pieces))
        level = level * jnp.repeat(jnp.exp(draws), dims[position] // blocks).reshape((-1,) + (1,) * (len(dims) - 1 - position))
    return level


def bell_draw(key, shape, scale, most, cuts=(), kind=jnp.bfloat16):
    drawn = scale * jax.random.normal(key, shape, jnp.float32)
    if cuts:
        drawn = drawn * shard_levels(key, shape, cuts, -0.22, 0.18)
    return jnp.clip(drawn, -most, most).astype(kind)


def setup_inputs(seed: int = 0) -> dict:
    streams_of = jax.random.split(jax.random.key(seed), 24)
    return {
        "tokens": bell_draw(streams_of[0], (TOKENS, D), 1.0, 6.0, ((0, 32),)),
        "mix_gain": jnp.clip(1.0 + 0.18 * jax.random.normal(streams_of[1], (D,), jnp.float32), 0.1, 1.9),
        "w_query": bell_draw(streams_of[2], (D, HEADS, HEAD), D ** -0.5, 0.125, ((1, 2), (2, 16))),
        "w_key": bell_draw(streams_of[3], (D, HEADS, HEAD), D ** -0.5, 0.125, ((1, 2), (2, 16))),
        "w_value": bell_draw(streams_of[4], (D, HEADS, HEAD), D ** -0.5, 0.125, ((1, 2), (2, 16))),
        "w_zgate": bell_draw(streams_of[5], (D, HEADS, HEAD), D ** -0.5, 0.125, ((1, 2), (2, 16))),
        "w_beta": bell_draw(streams_of[6], (D, HEADS), D ** -0.5, 0.125, ((1, 2),)),
        "w_decay": bell_draw(streams_of[7], (D, HEADS), D ** -0.5, 0.125, ((1, 2),)),
        "decay_rate": jnp.clip(jnp.exp(math.log(8.0) - 2.7725887 * jax.random.uniform(streams_of[8], (HEADS,), jnp.float32) ** shard_levels(streams_of[8], (HEADS,), ((0, 2),), -0.2, 0.2)), 0.5, 8.0),
        "decay_bias": jnp.clip(-3.0 + 3.0 * jax.random.uniform(streams_of[9], (HEADS,), jnp.float32) ** shard_levels(streams_of[9], (HEADS,), ((0, 2),), -0.2, 0.2), -3.0, 0.0),
        "head_gain": jnp.clip(1.0 + 0.18 * jax.random.normal(streams_of[10], (HEAD,), jnp.float32), 0.1, 1.9),
        "state": bell_draw(streams_of[11], (TOKENS, HEADS, HEAD, HEAD), 0.25, 1.5, ((0, 16), (1, 2)), jnp.float32),
        "w_out": bell_draw(streams_of[12], (HD, D), HD ** -0.5, 0.125, ((0, 2), (1, 16))),
        "moe_gain": jnp.clip(1.0 + 0.18 * jax.random.normal(streams_of[13], (D,), jnp.float32), 0.1, 1.9),
        "dense_mix": bell_draw(streams_of[14], (D,), D ** -0.5, 0.125),
        "dense_gate": bell_draw(streams_of[15], (D, FFD), D ** -0.5, 0.125, ((1, 32),)),
        "dense_up": bell_draw(streams_of[16], (D, FFD), D ** -0.5, 0.125, ((1, 32),)),
        "dense_down": bell_draw(streams_of[17], (FFD, D), FFD ** -0.5, 0.09375, ((0, 32),)),
        "expert_gate": bell_draw(streams_of[18], (EXPERTS, D, FFE), D ** -0.5, 0.125, ((0, 16), (2, 2))),
        "expert_up": bell_draw(streams_of[19], (EXPERTS, D, FFE), D ** -0.5, 0.125, ((0, 16), (2, 2))),
        "expert_down": bell_draw(streams_of[20], (EXPERTS, FFE, D), FFE ** -0.5, 0.1875, ((0, 16), (1, 2))),
        "expert_ids": draw_expert_ids(jax.random.fold_in(streams_of[23], 71), 0),
        "route_weight": jnp.clip(jnp.exp(jax.random.uniform(streams_of[22], (TOKENS, TOP_K), jnp.float32, math.log(0.1), math.log(1.0))), 0.1, 1.0),
    }


EPS = 1e-06

def rms_scale(values, gain):
    return values * lax.rsqrt(lax.optimization_barrier(jnp.mean(values * values, axis=-1, keepdims=True)) + EPS) * gain

def unit_rows(values):
    return values * lax.rsqrt(lax.optimization_barrier(jnp.sum(values * values, axis=-1, keepdims=True)) + EPS)

def reference(tokens, mix_gain, w_query, w_key, w_value, w_zgate, w_beta, w_decay, decay_rate, decay_bias, head_gain, state, w_out, moe_gain, dense_mix, dense_gate, dense_up, dense_down, expert_gate, expert_up, expert_down, expert_ids, route_weight):
    tok_float = tokens.astype(jnp.float32)
    normed = rms_scale(tok_float, mix_gain).astype(jnp.bfloat16)

    def project(weight):
        product = jnp.dot(normed, weight.reshape(D, HD), preferred_element_type=jnp.float32)
        return product.astype(jnp.bfloat16).reshape(TOKENS, HEADS, HEAD).astype(jnp.float32)
    query = unit_rows(jax.nn.silu(project(w_query))) * HEAD ** (-0.5)
    key_vec = unit_rows(jax.nn.silu(project(w_key)))
    value = jax.nn.silu(project(w_value))
    gate_in = project(w_zgate)
    beta_rate = jax.nn.sigmoid(jnp.dot(normed, w_beta, preferred_element_type=jnp.float32))
    decay_in = jnp.dot(normed, w_decay, preferred_element_type=jnp.float32)
    retain = jnp.exp(-decay_rate * jax.nn.softplus(decay_in + decay_bias))
    recalled = jnp.einsum('shkv,shk->shv', state, key_vec, precision=lax.Precision.HIGHEST)
    correction = value - retain[..., None] * recalled
    new_state = retain[..., None, None] * state + (beta_rate[..., None] * key_vec)[..., :, None] * correction[..., None, :]
    readout = jnp.einsum('shkv,shk->shv', new_state, query, precision=lax.Precision.HIGHEST)
    gated = rms_scale(readout, head_gain) * jax.nn.silu(gate_in)
    gated = gated.astype(jnp.bfloat16).reshape(TOKENS, HD)
    resid = tok_float + jnp.dot(gated, w_out, preferred_element_type=jnp.float32)
    moe_in = rms_scale(resid, moe_gain).astype(jnp.bfloat16)
    dense_hidden = (jax.nn.silu(jnp.dot(moe_in, dense_gate, preferred_element_type=jnp.float32)) * jnp.dot(moe_in, dense_up, preferred_element_type=jnp.float32)).astype(jnp.bfloat16)
    mix_factor = jax.nn.sigmoid(jnp.dot(moe_in, dense_mix, preferred_element_type=jnp.float32))
    dense_out = mix_factor[:, None] * jnp.dot(dense_hidden, dense_down, preferred_element_type=jnp.float32)
    positions = jnp.arange(TOKENS, dtype=jnp.int32)
    block_idx = positions // SEQ_GROUP
    slot_iota = jnp.arange(SLOTS, dtype=jnp.int32)

    def one_expert(summed, stacked):
        expert, gate_w, up_w, down_w = stacked
        matched = expert_ids == expert
        routed = jnp.any(matched, axis=1).astype(jnp.int32)
        weight = lax.optimization_barrier(jnp.sum(jnp.where(matched, route_weight, 0.0), axis=1))
        rank_in = (jnp.cumsum(routed.reshape(-1, SEQ_GROUP), axis=1).reshape(-1) - routed).astype(jnp.int32)
        slot_idx = (block_idx * CAP + rank_in).astype(jnp.int32)
        matches = (slot_idx[None, :] == slot_iota[:, None]) & (routed[None, :] > 0)
        source = lax.optimization_barrier(jnp.sum(jnp.where(matches, positions[None, :], 0), axis=1)).astype(jnp.int32)
        picked = jnp.take(moe_in, source, axis=0)
        expert_hidden = (jax.nn.silu(jnp.dot(picked, gate_w, preferred_element_type=jnp.float32)) * jnp.dot(picked, up_w, preferred_element_type=jnp.float32)).astype(jnp.bfloat16)
        expert_out = jnp.dot(expert_hidden, down_w, preferred_element_type=jnp.float32)
        row_take = jnp.take(expert_out, jnp.minimum(slot_idx, SLOTS - 1), axis=0)
        return (summed + weight[:, None] * row_take, None)
    moe_out, _ = lax.scan(one_expert, jnp.zeros((TOKENS, D), jnp.float32), (jnp.arange(EXPERTS, dtype=jnp.int32), expert_gate, expert_up, expert_down))
    layer_out = (resid + dense_out + moe_out).astype(jnp.bfloat16)
    return (layer_out, new_state)
```

```python
import functools

import jax
import jax.numpy as jnp
from jax import lax
from jax.experimental import pallas as pl
from jax.experimental.pallas import tpu as pltpu
from jax.sharding import PartitionSpec as P

EPS = 1e-06
VMEM = pltpu.VMEM
MESH = pl.DeviceIdType.MESH


def rms_scale(values, gain):
    return values * lax.rsqrt(jnp.mean(values * values, axis=-1, keepdims=True) + EPS) * gain


def grid_of(count):
    for depth in (4, 2, 1):
        side = int(round((count / depth) ** 0.5))
        if depth * side * side == count:
            return depth, side
    return count, 1


def place(count):
    depth, side = grid_of(count)
    ep = lax.axis_index("ep")
    t = lax.axis_index("tp")
    z = ep // (side * side)
    y = (ep // side) % side
    x = ep % side
    a = x * (1 - t) + y * t
    b = y * (1 - t) + x * t
    return depth, side, t, z, b, a


def ep_of(side, t, z, b, a):
    y = b * (1 - t) + a * t
    x = a * (1 - t) + b * t
    return (z * side + y) * side + x


def greet(devices):
    barrier = pltpu.get_barrier_semaphore()
    for device in devices:
        pl.semaphore_signal(barrier, inc=1, device_id=device, device_id_type=MESH)
    pl.semaphore_wait(barrier, len(devices))


def gather_kernel(count, both, block_ref, out_ref, send_sem, recv_sem):
    depth, side, t, z, b, a = place(count)
    zs = [((lax.rem(z + i, depth)), b, a) for i in range(1, depth)]
    bs = [(z, lax.rem(b + i, side), a) for i in range(1, side)]
    as_ = [(z, b, lax.rem(a + i, side)) for i in range(1, side)]
    device_of = lambda c: (ep_of(side, t, *c), t)
    peers = [device_of(c) for c in zs + bs + as_]
    partner = (lax.axis_index("ep"), 1 - t)
    greet(peers + ([partner] if both else []))
    width = 2 if both else 1
    slot_of = lambda dz, db, da: (
        ep_of(side, t, lax.rem(z + dz, depth), lax.rem(b + db, side), lax.rem(a + da, side)) * width
        + (t if both else 0)
    )
    mine = slot_of(0, 0, 0)
    out_ref[mine] = block_ref[...]
    counter = [0]
    started = []
    arrivals = {}

    def send(src, offset, key, device):
        number = counter[0]
        counter[0] += 1
        copy = pltpu.make_async_remote_copy(
            src_ref=src,
            dst_ref=out_ref.at[slot_of(*offset)],
            send_sem=send_sem.at[number],
            recv_sem=recv_sem.at[number],
            device_id=device,
            device_id_type=MESH,
        )
        copy.start()
        started.append(copy)
        arrivals[key] = copy

    def relay(offset, legs):
        dz, db, da = offset
        src = block_ref if offset == (0, 0, 0) else out_ref.at[slot_of(*offset)]
        if "a" in legs:
            for i in range(1, side):
                send(src, offset, ("a", (dz, db, (da - i) % side)), device_of(as_[i - 1]))
        if "b" in legs:
            for i in range(1, side):
                send(src, offset, ("b", (dz, (db - i) % side, da)), device_of(bs[i - 1]))
        if "z" in legs:
            for i in range(1, depth):
                send(src, offset, ("z", ((dz - i) % depth, db, da)), device_of(zs[i - 1]))
        if both:
            send(src, offset, ("t", offset), partner)

    relay((0, 0, 0), "zba")
    for dz in range(1, depth):
        arrivals["z", (dz, 0, 0)].wait_recv()
        relay((dz, 0, 0), "ba")
    for dz in range(depth):
        for db in range(1, side):
            arrivals["b", (dz, db, 0)].wait_recv()
            relay((dz, db, 0), "a")
    for dz in range(depth):
        for db in range(side):
            for da in range(1, side):
                arrivals["a", (dz, db, da)].wait_recv()
                relay((dz, db, da), "")
    if both:
        for key, copy in arrivals.items():
            if key[0] == "t":
                copy.wait_recv()
    for copy in started:
        copy.wait_send()


def gather(block, count, both, number):
    total = count * (2 if both else 1)
    depth, side = grid_of(count)
    copies = count - 1 + (count if both else 0)
    return pl.pallas_call(
        functools.partial(gather_kernel, count, both),
        out_shape=jax.ShapeDtypeStruct((total,) + block.shape, block.dtype),
        in_specs=[pl.BlockSpec(memory_space=VMEM)],
        out_specs=pl.BlockSpec(memory_space=VMEM),
        scratch_shapes=[
            pltpu.SemaphoreType.DMA((copies,)),
            pltpu.SemaphoreType.DMA((copies,)),
        ],
        compiler_params=pltpu.CompilerParams(collective_id=number, has_side_effects=True),
        name=f"gather_{number}",
    )(block)


def exchange_kernel(count, both, blocks_ref, out_ref, send_sem, recv_sem):
    ep = lax.axis_index("ep")
    t = lax.axis_index("tp")
    total = count * 2 if both else count
    me = ep * 2 + t if both else ep

    def device(i):
        other = lax.rem(me + i, total)
        return other, ((other // 2, other % 2) if both else (other, t))

    barrier = pltpu.get_barrier_semaphore()

    def hello(i, carry):
        pl.semaphore_signal(barrier, inc=1, device_id=device(i)[1], device_id_type=MESH)
        return carry

    lax.fori_loop(1, total, hello, 0)
    pl.semaphore_wait(barrier, total - 1)

    def copy(i):
        other, target = device(i)
        return pltpu.make_async_remote_copy(
            src_ref=blocks_ref.at[other],
            dst_ref=out_ref.at[me],
            send_sem=send_sem.at[i],
            recv_sem=recv_sem.at[i],
            device_id=target,
            device_id_type=MESH,
        )

    def start(i, carry):
        copy(i).start()
        return carry

    def finish(i, carry):
        copy(i).wait()
        return carry

    lax.fori_loop(1, total, start, 0)
    out_ref[me] = blocks_ref[me]
    lax.fori_loop(1, total, finish, 0)


def exchange(blocks, count, both, number):
    return pl.pallas_call(
        functools.partial(exchange_kernel, count, both),
        out_shape=jax.ShapeDtypeStruct(blocks.shape, blocks.dtype),
        in_specs=[pl.BlockSpec(memory_space=VMEM)],
        out_specs=pl.BlockSpec(memory_space=VMEM),
        scratch_shapes=[
            pltpu.SemaphoreType.DMA((blocks.shape[0],)),
            pltpu.SemaphoreType.DMA((blocks.shape[0],)),
        ],
        compiler_params=pltpu.CompilerParams(collective_id=number, has_side_effects=True),
        name=f"exchange_{number}",
    )(blocks)


def scatter_kernel(
    count, part_ref, out_ref, core_buf, sum1, a_buf, sum2, b_buf, sum3, z_buf, send_sem, recv_sem
):
    depth, side, t, z, b, a = place(count)
    device_of = lambda dz, db, da: (
        ep_of(side, t, lax.rem(z + dz, depth), lax.rem(b + db, side), lax.rem(a + da, side)),
        t,
    )
    partner = (lax.axis_index("ep"), 1 - t)
    greet(
        [partner]
        + [device_of(i, 0, 0) for i in range(1, depth)]
        + [device_of(0, i, 0) for i in range(1, side)]
        + [device_of(0, 0, i) for i in range(1, side)]
    )
    flat = lambda core, dz, db, da: (
        ep_of(side, t, lax.rem(z + dz, depth), lax.rem(b + db, side), lax.rem(a + da, side)) * 2
        + core
    )
    counter = [0]
    started = []

    def send(src, dst, device, number=None):
        if number is None:
            number = count + counter[0]
            counter[0] += 1
        copy = pltpu.make_async_remote_copy(
            src_ref=src,
            dst_ref=dst,
            send_sem=send_sem.at[number],
            recv_sem=recv_sem.at[number],
            device_id=device,
            device_id_type=MESH,
        )
        copy.start()
        started.append(copy)
        return copy

    add = lambda first, *rest: functools.reduce(
        lambda u, v: u + v, [w.astype(jnp.float32) for w in (first,) + rest]
    )
    order = [
        (dz, db, da)
        for da in list(range(1, side)) + [0]
        for db in list(range(1, side)) + [0]
        for dz in list(range(1, depth)) + [0]
    ]
    absolute = lambda dz, db, da: ep_of(
        side, t, lax.rem(z + dz, depth), lax.rem(b + db, side), lax.rem(a + da, side)
    )
    for dz, db, da in order:
        spot = absolute(dz, da, db)
        send(part_ref.at[spot * 2 + 1 - t], core_buf.at[spot], partner, spot)

    def core_arrival(spot):
        return pltpu.make_async_remote_copy(
            src_ref=part_ref.at[spot * 2 + 1 - t],
            dst_ref=core_buf.at[spot],
            send_sem=send_sem.at[spot],
            recv_sem=recv_sem.at[spot],
            device_id=partner,
            device_id_type=MESH,
        )

    a_copies = {}
    for c in order:
        dz, db, da = c
        core_arrival(absolute(*c)).wait_recv()
        total = add(part_ref[absolute(*c) * 2 + t], core_buf[absolute(*c)])
        slot = (da * side + db) * depth + dz
        sum1[slot] = total.astype(sum1.dtype)
        if da:
            a_copies[c] = send(
                sum1.at[slot], a_buf.at[(da * side + db) * depth + dz], device_of(0, 0, da)
            )
    b_copies = {}
    for db in list(range(1, side)) + [0]:
        for dz in list(range(1, depth)) + [0]:
            terms = [sum1[db * depth + dz]]
            for da in range(1, side):
                a_copies[dz, db, da].wait_recv()
                terms.append(a_buf[(da * side + db) * depth + dz])
            sum2[db * depth + dz] = add(*terms).astype(sum2.dtype)
            if db:
                b_copies[dz, db] = send(
                    sum2.at[db * depth + dz], b_buf.at[db * depth + dz], device_of(0, db, 0)
                )
    z_copies = []
    for dz in list(range(1, depth)) + [0]:
        terms = [sum2[dz]]
        for db in range(1, side):
            b_copies[dz, db].wait_recv()
            terms.append(b_buf[db * depth + dz])
        total = add(*terms)
        if dz:
            sum3[dz] = total.astype(sum3.dtype)
            z_copies.append(send(sum3.at[dz], z_buf.at[dz], device_of(dz, 0, 0)))
    for dz in range(1, depth):
        z_copies[dz - 1].wait_recv()
        total = total + z_buf[dz].astype(jnp.float32)
    out_ref[...] = total
    for copy in started:
        copy.wait_send()


def scatter(parts, count, number):
    depth, side = grid_of(count)
    block = parts.shape[1:]
    copies = count + (side - 1) * side * depth + (side - 1) * depth + depth - 1
    buf = lambda n: pltpu.VMEM((n,) + block, parts.dtype)
    return pl.pallas_call(
        functools.partial(scatter_kernel, count),
        out_shape=jax.ShapeDtypeStruct(block, jnp.float32),
        in_specs=[pl.BlockSpec(memory_space=VMEM)],
        out_specs=pl.BlockSpec(memory_space=VMEM),
        scratch_shapes=[
            buf(count),
            buf(count),
            buf(count),
            buf(side * depth),
            buf(side * depth),
            buf(depth),
            buf(depth),
            pltpu.SemaphoreType.DMA((copies,)),
            pltpu.SemaphoreType.DMA((copies,)),
        ],
        compiler_params=pltpu.CompilerParams(collective_id=number, has_side_effects=True),
        name=f"scatter_{number}",
    )(parts)


def delta_kernel(heads, rows_ref, cols_ref, retain_ref, beta_ref, gain_ref, state_ref, gated_ref, new_ref):
    head_size = cols_ref.shape[1]
    silu = lambda v: v / (1.0 + jnp.exp(-v))
    cols = silu(cols_ref[0])
    cols = cols * lax.rsqrt(jnp.sum(cols * cols, axis=0, keepdims=True) + EPS)
    rows = silu(rows_ref[0])
    value, gate = rows[:heads], rows[heads:]
    readouts = []
    for h in range(heads):
        query = cols[:, h : h + 1] * head_size ** (-0.5)
        key = cols[:, heads + h : heads + h + 1]
        keep = retain_ref[0, h : h + 1, :]
        old = state_ref[0, h]
        recalled = jnp.sum(old * key, axis=0, keepdims=True)
        correction = value[h : h + 1] - keep * recalled
        new = keep * old + key * (beta_ref[0, h : h + 1, :] * correction)
        new_ref[0, h] = new
        readouts.append(jnp.sum(new * query, axis=0, keepdims=True))
    readout = jnp.concatenate(readouts, axis=0)
    gated = rms_scale(readout, gain_ref[...]) * gate
    gated_ref[0] = gated.astype(gated_ref.dtype)


def delta(rows, cols, retain, beta, gain, state):
    seqs, heads, size, _ = state.shape
    own = lambda *shape: pl.BlockSpec((1,) + shape, lambda s: (s,) + (0,) * len(shape))
    return pl.pallas_call(
        functools.partial(delta_kernel, heads),
        grid=(seqs,),
        out_shape=(
            jax.ShapeDtypeStruct((seqs, heads, size), jnp.bfloat16),
            jax.ShapeDtypeStruct(state.shape, state.dtype),
        ),
        in_specs=[
            own(2 * heads, size),
            own(size, 2 * heads),
            own(heads, size),
            own(heads, size),
            pl.BlockSpec((1, size), lambda s: (0, 0)),
            own(heads, size, size),
        ],
        out_specs=(own(heads, size), own(heads, size, size)),
        compiler_params=pltpu.CompilerParams(dimension_semantics=("arbitrary",)),
        name="delta",
    )(rows, cols, retain, beta, gain.reshape(1, size), state)


def body(
    tokens,
    mix_gain,
    w_query,
    w_key,
    w_value,
    w_zgate,
    w_beta,
    w_decay,
    decay_rate,
    decay_bias,
    head_gain,
    state,
    w_out,
    moe_gain,
    dense_mix,
    dense_gate,
    dense_up,
    dense_down,
    expert_gate,
    expert_up,
    expert_down,
    expert_ids,
    route_weight,
):
    ep_count = lax.axis_size("ep")
    group_idx = lax.axis_index("ep")
    own_rows, width = tokens.shape
    seqs, heads, size, _ = state.shape
    part = w_query.shape[2]
    total_rows = ep_count * seqs
    tok_float = tokens.astype(jnp.float32)
    normed = rms_scale(tok_float, mix_gain).astype(jnp.bfloat16)
    rows_all = gather(normed, ep_count, True, 1).reshape(total_rows, width)
    w_cat = jnp.stack([w_query, w_key, w_value, w_zgate], axis=1).reshape(width, -1)
    projected = jnp.dot(rows_all, w_cat, preferred_element_type=jnp.float32)
    projected = projected.astype(jnp.bfloat16).reshape(ep_count, seqs, -1)
    swapped = exchange(projected, ep_count, False, 2)
    swapped = swapped.reshape(ep_count, seqs, 2, 2 * heads, part).astype(jnp.float32)
    cols = swapped[:, :, 0].transpose(1, 0, 3, 2).reshape(seqs, size, 2 * heads)
    rows = swapped[:, :, 1].transpose(1, 2, 0, 3).reshape(seqs, 2 * heads, size)
    seq_rows = lax.dynamic_slice_in_dim(rows_all, group_idx * seqs, seqs, 0)
    rates = jnp.dot(
        seq_rows, jnp.concatenate([w_beta, w_decay], axis=1), preferred_element_type=jnp.float32
    )
    beta_rate = jax.nn.sigmoid(rates[:, :heads])
    retain = jnp.exp(-decay_rate * jax.nn.softplus(rates[:, heads:] + decay_bias))
    spread = lambda v: jnp.broadcast_to(v[:, :, None], (seqs, heads, size))
    gated, new_state = delta(rows, cols, spread(retain), spread(beta_rate), head_gain, state)
    gated_all = gather(gated.reshape(seqs, heads * size), ep_count, False, 3)
    partial_value = jnp.dot(
        gated_all.reshape(total_rows, heads * size), w_out, preferred_element_type=jnp.float32
    )
    partial_value = partial_value.astype(jnp.bfloat16).reshape(-1, own_rows, w_out.shape[1])
    mixed = exchange(partial_value, ep_count, True, 4).astype(jnp.float32)
    mixed = mixed.reshape(ep_count, -1, own_rows, w_out.shape[1]).sum(axis=1)
    resid = tok_float + mixed.transpose(1, 0, 2).reshape(own_rows, width)
    moe_in = rms_scale(resid, moe_gain).astype(jnp.bfloat16)
    moe_all = gather(moe_in, ep_count, True, 5).reshape(total_rows, width)

    def branch(gate, up, down):
        hidden = jax.nn.silu(jnp.dot(moe_all, gate, preferred_element_type=jnp.float32))
        hidden = hidden * jnp.dot(moe_all, up, preferred_element_type=jnp.float32)
        return jnp.dot(hidden.astype(jnp.bfloat16), down, preferred_element_type=jnp.float32)

    mix_factor = jax.nn.sigmoid(jnp.dot(moe_all, dense_mix, preferred_element_type=jnp.float32))
    weight = jnp.sum(jnp.where(expert_ids == group_idx, route_weight, 0.0), axis=1)
    terms = mix_factor[:, None] * branch(dense_gate, dense_up, dense_down)
    terms = terms + weight[:, None] * branch(expert_gate[0], expert_up[0], expert_down[0])
    terms = terms.astype(jnp.bfloat16).reshape(-1, own_rows, width)
    layer_out = (resid + scatter(terms, ep_count, 6)).astype(jnp.bfloat16)
    return (layer_out, new_state)


def solution(mesh):
    placed = (
        P(("ep", "tp"), None),
        P(),
        P(None, "tp", "ep"),
        P(None, "tp", "ep"),
        P(None, "tp", "ep"),
        P(None, "tp", "ep"),
        P(None, "tp"),
        P(None, "tp"),
        P("tp"),
        P("tp"),
        P(),
        P("ep", "tp", None, None),
        P("tp", "ep"),
        P(),
        P(),
        P(None, ("ep", "tp")),
        P(None, ("ep", "tp")),
        P(("ep", "tp"), None),
        P("ep", None, "tp"),
        P("ep", None, "tp"),
        P("ep", "tp", None),
        P(),
        P(),
    )
    return jax.shard_map(
        body,
        mesh=mesh,
        in_specs=placed,
        out_specs=(P(("ep", "tp"), None), P("ep", "tp", None, None)),
        check_vma=False,
    )
```

```python
import functools

import jax
import jax.numpy as jnp
from jax import lax
from jax.experimental import pallas as pl
from jax.experimental.pallas import tpu as pltpu
from jax.sharding import PartitionSpec as P

EPS = 1e-06
VMEM = pltpu.VMEM
MESH = pl.DeviceIdType.MESH


def rms_scale(values, gain):
    return values * lax.rsqrt(jnp.mean(values * values, axis=-1, keepdims=True) + EPS) * gain


def grid_of(count):
    for depth in (4, 2, 1):
        side = int(round((count / depth) ** 0.5))
        if depth * side * side == count:
            return depth, side
    return count, 1


def place(count):
    depth, side = grid_of(count)
    ep = lax.axis_index("ep")
    t = lax.axis_index("tp")
    z = ep // (side * side)
    y = (ep // side) % side
    x = ep % side
    a = x * (1 - t) + y * t
    b = y * (1 - t) + x * t
    return depth, side, t, z, b, a


def ep_of(side, t, z, b, a):
    y = b * (1 - t) + a * t
    x = a * (1 - t) + b * t
    return (z * side + y) * side + x


def near(count):
    depth, side, t, z, b, a = place(count)
    steps = [(lax.rem(z + i, depth), b, a) for i in range(1, depth)]
    steps += [(z, lax.rem(b + i, side), a) for i in range(1, side)]
    steps += [(z, b, lax.rem(a + i, side)) for i in range(1, side)]
    return [(ep_of(side, t, *c), t) for c in steps]


def gather_phase(count, both, block_ref, out_ref, send_sem, recv_sem):
    depth, side, t, z, b, a = place(count)
    zs = [((lax.rem(z + i, depth)), b, a) for i in range(1, depth)]
    bs = [(z, lax.rem(b + i, side), a) for i in range(1, side)]
    as_ = [(z, b, lax.rem(a + i, side)) for i in range(1, side)]
    device_of = lambda c: (ep_of(side, t, *c), t)
    partner = (lax.axis_index("ep"), 1 - t)
    width = 2 if both else 1
    slot_of = lambda dz, db, da: (
        ep_of(side, t, lax.rem(z + dz, depth), lax.rem(b + db, side), lax.rem(a + da, side)) * width
        + (t if both else 0)
    )
    mine = slot_of(0, 0, 0)
    out_ref[mine] = block_ref[...]
    counter = [0]
    started = []
    arrivals = {}

    def send(src, offset, key, device):
        number = counter[0]
        counter[0] += 1
        copy = pltpu.make_async_remote_copy(
            src_ref=src,
            dst_ref=out_ref.at[slot_of(*offset)],
            send_sem=send_sem.at[number],
            recv_sem=recv_sem.at[number],
            device_id=device,
            device_id_type=MESH,
        )
        copy.start()
        started.append(copy)
        arrivals[key] = copy

    def relay(offset, legs):
        dz, db, da = offset
        src = block_ref if offset == (0, 0, 0) else out_ref.at[slot_of(*offset)]
        if "a" in legs:
            for i in range(1, side):
                send(src, offset, ("a", (dz, db, (da - i) % side)), device_of(as_[i - 1]))
        if "b" in legs:
            for i in range(1, side):
                send(src, offset, ("b", (dz, (db - i) % side, da)), device_of(bs[i - 1]))
        if "z" in legs:
            for i in range(1, depth):
                send(src, offset, ("z", ((dz - i) % depth, db, da)), device_of(zs[i - 1]))
        if both:
            send(src, offset, ("t", offset), partner)

    relay((0, 0, 0), "zba")
    for dz in range(1, depth):
        arrivals["z", (dz, 0, 0)].wait_recv()
        relay((dz, 0, 0), "ba")
    for dz in range(depth):
        for db in range(1, side):
            arrivals["b", (dz, db, 0)].wait_recv()
            relay((dz, db, 0), "a")
    for dz in range(depth):
        for db in range(side):
            for da in range(1, side):
                arrivals["a", (dz, db, da)].wait_recv()
                relay((dz, db, da), "")
    if both:
        for key, copy in arrivals.items():
            if key[0] == "t":
                copy.wait_recv()
    for copy in started:
        copy.wait_send()


def copies_of(count, both):
    return count - 1 + (count if both else 0)


def device_at(count, both, i):
    t = lax.axis_index("tp")
    me = lax.axis_index("ep") * 2 + t if both else lax.axis_index("ep")
    other = lax.rem(me + i, count * 2 if both else count)
    return other, ((other // 2, other % 2) if both else (other, t))


def greet_all(count, both):
    barrier = pltpu.get_barrier_semaphore()

    def hello(i, carry):
        pl.semaphore_signal(
            barrier, inc=1, device_id=device_at(count, both, i)[1], device_id_type=MESH
        )
        return carry

    lax.fori_loop(1, count * 2 if both else count, hello, 0)


def exchange_phase(count, both, blocks_ref, out_ref, send_sem, recv_sem):
    total = count * 2 if both else count
    t = lax.axis_index("tp")
    me = lax.axis_index("ep") * 2 + t if both else lax.axis_index("ep")

    def copy(i):
        other, target = device_at(count, both, i)
        return pltpu.make_async_remote_copy(
            src_ref=blocks_ref.at[other],
            dst_ref=out_ref.at[me],
            send_sem=send_sem.at[i],
            recv_sem=recv_sem.at[i],
            device_id=target,
            device_id_type=MESH,
        )

    def start(i, carry):
        copy(i).start()
        return carry

    def finish(i, carry):
        copy(i).wait()
        return carry

    lax.fori_loop(1, total, start, 0)
    out_ref[me] = blocks_ref[me]
    lax.fori_loop(1, total, finish, 0)


def contract(left, right):
    return lax.dot_general(left, right, (((1,), (1,)), ((), ())), preferred_element_type=jnp.float32)


def flat_rows(ref):
    blocks, rows, width = ref.shape
    return ref[...].astype(jnp.float32).reshape(blocks * rows, width)


def project_kernel(
    count,
    tokens_ref,
    gain_ref,
    wq_ref,
    wk_ref,
    wv_ref,
    wz_ref,
    beta_ref,
    decay_ref,
    out_ref,
    rates_ref,
    own,
    rows,
    blocks,
    send_sem,
    recv_sem,
    send_sem2,
    recv_sem2,
):
    partner = (lax.axis_index("ep"), 1 - lax.axis_index("tp"))
    barrier = pltpu.get_barrier_semaphore()
    pl.semaphore_signal(barrier, inc=1, device_id=partner, device_id_type=MESH)
    greet_all(count, False)
    own[...] = rms_scale(tokens_ref[...].astype(jnp.float32), gain_ref[...]).astype(own.dtype)
    pl.semaphore_wait(barrier, count)
    gather_phase(count, True, own, rows, send_sem, recv_sem)
    flat = flat_rows(rows).astype(jnp.bfloat16)
    heads = beta_ref.shape[0]
    columns = wq_ref.shape[0]
    wide = 4 * columns
    source = lax.broadcasted_iota(jnp.int32, (columns, wide), 0)
    target = lax.broadcasted_iota(jnp.int32, (columns, wide), 1)
    moved = jnp.zeros((flat.shape[0], wide), jnp.float32)
    for p, w_ref in enumerate((wq_ref, wk_ref, wv_ref, wz_ref)):
        piece = contract(flat, w_ref[...]).astype(jnp.bfloat16)
        spot = source % (columns // heads) * (4 * heads) + p * heads + source // (columns // heads)
        order = jnp.where(target == spot, 1.0, 0.0).astype(jnp.bfloat16)
        moved = moved + jnp.dot(piece, order, preferred_element_type=jnp.float32)
    blocks[...] = moved.reshape(blocks.shape).astype(blocks.dtype)
    ep = lax.axis_index("ep")
    seq = jnp.concatenate(
        [rows[2 * ep].astype(jnp.float32), rows[2 * ep + 1].astype(jnp.float32)], axis=0
    ).astype(jnp.bfloat16)
    exchange_phase(count, False, blocks, out_ref, send_sem2, recv_sem2)
    rates_ref[:, :heads] = contract(seq, beta_ref[...])
    rates_ref[:, heads:] = contract(seq, decay_ref[...])


def sems(n):
    return [pltpu.SemaphoreType.DMA((n,)), pltpu.SemaphoreType.DMA((n,))]


def comm_call(kernel, number, out_shape, operands, scratch):
    spec = pl.BlockSpec(memory_space=VMEM)
    return pl.pallas_call(
        kernel,
        out_shape=out_shape,
        in_specs=[spec] * len(operands),
        out_specs=jax.tree.map(lambda _: spec, out_shape),
        scratch_shapes=scratch,
        compiler_params=pltpu.CompilerParams(
            collective_id=number, has_side_effects=True, vmem_limit_bytes=60 * 1024 * 1024
        ),
        name=f"stage_{number}",
    )(*operands)


def mix_kernel(
    count,
    gated_ref,
    w_ref,
    tokens_ref,
    gain_ref,
    resid_ref,
    all_ref,
    rows,
    parts,
    landed,
    own,
    send_sem,
    recv_sem,
    send_sem2,
    recv_sem2,
    send_sem3,
    recv_sem3,
):
    greet_all(count, True)
    pl.semaphore_wait(pltpu.get_barrier_semaphore(), 2 * count - 1)
    gather_phase(count, False, gated_ref, rows, send_sem, recv_sem)
    flat = flat_rows(rows).astype(jnp.bfloat16)
    product = jnp.dot(flat, w_ref[...], preferred_element_type=jnp.float32)
    parts[...] = product.reshape(parts.shape).astype(parts.dtype)
    exchange_phase(count, True, parts, landed, send_sem2, recv_sem2)
    mixed = [
        landed[2 * i].astype(jnp.float32) + landed[2 * i + 1].astype(jnp.float32)
        for i in range(count)
    ]
    resid = tokens_ref[...].astype(jnp.float32) + jnp.concatenate(mixed, axis=1)
    resid_ref[...] = resid
    own[...] = rms_scale(resid, gain_ref[...]).astype(own.dtype)
    gather_phase(count, True, own, all_ref, send_sem3, recv_sem3)


def scatter_phase(
    count, part_ref, core_buf, sum1, a_buf, sum2, b_buf, sum3, z_buf, send_sem, recv_sem
):
    depth, side, t, z, b, a = place(count)
    device_of = lambda dz, db, da: (
        ep_of(side, t, lax.rem(z + dz, depth), lax.rem(b + db, side), lax.rem(a + da, side)),
        t,
    )
    partner = (lax.axis_index("ep"), 1 - t)
    counter = [0]
    started = []

    def send(src, dst, device, number=None):
        if number is None:
            number = count + counter[0]
            counter[0] += 1
        copy = pltpu.make_async_remote_copy(
            src_ref=src,
            dst_ref=dst,
            send_sem=send_sem.at[number],
            recv_sem=recv_sem.at[number],
            device_id=device,
            device_id_type=MESH,
        )
        copy.start()
        started.append(copy)
        return copy

    add = lambda first, *rest: functools.reduce(
        lambda u, v: u + v, [w.astype(jnp.float32) for w in (first,) + rest]
    )
    order = [
        (dz, db, da)
        for da in list(range(1, side)) + [0]
        for db in list(range(1, side)) + [0]
        for dz in list(range(1, depth)) + [0]
    ]
    absolute = lambda dz, db, da: ep_of(
        side, t, lax.rem(z + dz, depth), lax.rem(b + db, side), lax.rem(a + da, side)
    )
    for dz, db, da in order:
        spot = absolute(dz, da, db)
        send(part_ref.at[spot * 2 + 1 - t], core_buf.at[spot], partner, spot)

    def core_arrival(spot):
        return pltpu.make_async_remote_copy(
            src_ref=part_ref.at[spot * 2 + 1 - t],
            dst_ref=core_buf.at[spot],
            send_sem=send_sem.at[spot],
            recv_sem=recv_sem.at[spot],
            device_id=partner,
            device_id_type=MESH,
        )

    a_copies = {}
    for c in order:
        dz, db, da = c
        core_arrival(absolute(*c)).wait_recv()
        total = add(part_ref[absolute(*c) * 2 + t], core_buf[absolute(*c)])
        slot = (da * side + db) * depth + dz
        sum1[slot] = total.astype(sum1.dtype)
        if da:
            a_copies[c] = send(
                sum1.at[slot], a_buf.at[(da * side + db) * depth + dz], device_of(0, 0, da)
            )
    b_copies = {}
    for db in list(range(1, side)) + [0]:
        for dz in list(range(1, depth)) + [0]:
            terms = [sum1[db * depth + dz]]
            for da in range(1, side):
                a_copies[dz, db, da].wait_recv()
                terms.append(a_buf[(da * side + db) * depth + dz])
            sum2[db * depth + dz] = add(*terms).astype(sum2.dtype)
            if db:
                b_copies[dz, db] = send(
                    sum2.at[db * depth + dz], b_buf.at[db * depth + dz], device_of(0, db, 0)
                )
    z_copies = []
    for dz in list(range(1, depth)) + [0]:
        terms = [sum2[dz]]
        for db in range(1, side):
            b_copies[dz, db].wait_recv()
            terms.append(b_buf[db * depth + dz])
        total = add(*terms)
        if dz:
            sum3[dz] = total.astype(sum3.dtype)
            z_copies.append(send(sum3.at[dz], z_buf.at[dz], device_of(dz, 0, 0)))
    for dz in range(1, depth):
        z_copies[dz - 1].wait_recv()
        total = total + z_buf[dz].astype(jnp.float32)
    for copy in started:
        copy.wait_send()
    return total


def moe_kernel(
    count,
    rows_ref,
    resid_ref,
    mix_ref,
    dg_ref,
    du_ref,
    dd_ref,
    eg_ref,
    eu_ref,
    ed_ref,
    ids_ref,
    route_ref,
    out_ref,
    part,
    *rest,
):
    ep = lax.axis_index("ep")
    partner = (ep, 1 - lax.axis_index("tp"))
    barrier = pltpu.get_barrier_semaphore()
    peers = [partner] + near(count)
    for device in peers:
        pl.semaphore_signal(barrier, inc=1, device_id=device, device_id_type=MESH)
    wide = flat_rows(rows_ref)
    total, width = wide.shape
    mix = 1.0 / (1.0 + jnp.exp(-jnp.sum(wide * mix_ref[...], axis=1, keepdims=True)))
    flat = wide.astype(jnp.bfloat16)
    weight = jnp.sum(jnp.where(ids_ref[...] == ep, route_ref[...], 0.0), axis=0, keepdims=True)
    line = lax.broadcasted_iota(jnp.int32, (total, total), 0)
    lane = lax.broadcasted_iota(jnp.int32, (total, total), 1)
    weight = jnp.sum(jnp.where(line == lane, weight, 0.0), axis=1, keepdims=True)

    def hidden(gate, up):
        gate = jnp.dot(flat, gate, preferred_element_type=jnp.float32)
        up = jnp.dot(flat, up, preferred_element_type=jnp.float32)
        return (gate / (1.0 + jnp.exp(-gate)) * up).astype(jnp.bfloat16)

    dense = hidden(dg_ref[...], du_ref[...])
    expert = hidden(eg_ref[...], eu_ref[...])
    step = min(512, width)
    for start in range(0, width, step):
        span = slice(start, start + step)
        term = mix * jnp.dot(dense, dd_ref[:, span], preferred_element_type=jnp.float32)
        term = term + weight * jnp.dot(expert, ed_ref[:, span], preferred_element_type=jnp.float32)
        part[:, :, span] = term.reshape(part.shape[0], part.shape[1], step).astype(part.dtype)
    pl.semaphore_wait(barrier, len(peers))
    total = scatter_phase(count, part, *rest)
    out_ref[...] = (resid_ref[...] + total).astype(out_ref.dtype)


def delta_kernel(
    heads, rate_ref, bias_ref, rates_ref, x_ref, gain_ref, state_ref, gated_ref, new_ref, cols_buf, acc
):
    seq = pl.program_id(0)
    count, wide = x_ref.shape[1:]
    part = wide // (4 * heads)
    size = count * part
    silu = lambda v: v / (1.0 + jnp.exp(-v))
    x = x_ref[0]
    for i in range(part):
        cols_buf[pl.ds(i, count, stride=part), :] = x[:, i * 4 * heads : (i + 1) * 4 * heads]
    cols = cols_buf[...]
    rows = silu(jnp.transpose(cols)[2 * heads :])
    cols = silu(cols)
    cols = cols * lax.rsqrt(jnp.sum(cols * cols, axis=0, keepdims=True) + EPS)
    value, gate = rows[:heads], rows[heads:]
    tall = lambda pick: jnp.concatenate(
        [jnp.full((1, size), pick(h), jnp.float32) for h in range(heads)], axis=0
    )
    beta = 1.0 / (1.0 + jnp.exp(-tall(lambda h: rates_ref[seq, h])))
    pre = tall(lambda h: rates_ref[seq, heads + h] + bias_ref[h])
    soft = jnp.maximum(pre, 0.0) + jnp.log1p(jnp.exp(-jnp.abs(pre)))
    retain = jnp.exp(-tall(lambda h: rate_ref[h]) * soft)
    readouts = []
    for h in range(heads):
        query = cols[:, h : h + 1] * size ** (-0.5)
        key = cols[:, heads + h : heads + h + 1]
        keep = retain[h : h + 1]
        old = state_ref[0, h]
        recalled = jnp.sum(old * key, axis=0, keepdims=True)
        correction = value[h : h + 1] - keep * recalled
        new = keep * old + key * (beta[h : h + 1] * correction)
        new_ref[0, h] = new
        readouts.append(jnp.sum(new * query, axis=0, keepdims=True))
    readout = jnp.concatenate(readouts, axis=0)
    gated = rms_scale(readout, gain_ref[...]) * gate
    acc[pl.ds(pl.multiple_of(seq * heads, heads), heads), :] = gated

    @pl.when(seq == pl.num_programs(0) - 1)
    def _():
        for h in range(heads):
            piece = acc[pl.ds(h, gated_ref.shape[0], stride=heads), :]
            gated_ref[:, h * size : (h + 1) * size] = piece.astype(gated_ref.dtype)


def delta(rate, bias, rates, x, gain, state):
    seqs, heads, size, _ = state.shape
    own = lambda *shape: pl.BlockSpec((1,) + shape, lambda s: (s,) + (0,) * len(shape))
    scalars = pl.BlockSpec(memory_space=pltpu.SMEM)
    return pl.pallas_call(
        functools.partial(delta_kernel, heads),
        grid=(seqs,),
        out_shape=(
            jax.ShapeDtypeStruct((seqs, heads * size), jnp.bfloat16),
            jax.ShapeDtypeStruct(state.shape, state.dtype),
        ),
        in_specs=[
            scalars,
            scalars,
            scalars,
            own(*x.shape[1:]),
            pl.BlockSpec((1, size), lambda s: (0, 0)),
            own(heads, size, size),
        ],
        out_specs=(
            pl.BlockSpec((seqs, heads * size), lambda s: (0, 0)),
            own(heads, size, size),
        ),
        scratch_shapes=[
            pltpu.VMEM((size, 4 * heads), jnp.float32),
            pltpu.VMEM((seqs * heads, size), jnp.float32),
        ],
        compiler_params=pltpu.CompilerParams(dimension_semantics=("arbitrary",)),
        name="delta",
    )(rate, bias, rates, x, gain.reshape(1, size), state)


def body(
    tokens,
    mix_gain,
    w_query,
    w_key,
    w_value,
    w_zgate,
    w_beta,
    w_decay,
    decay_rate,
    decay_bias,
    head_gain,
    state,
    w_out,
    moe_gain,
    dense_mix,
    dense_gate,
    dense_up,
    dense_down,
    expert_gate,
    expert_up,
    expert_down,
    expert_ids,
    route_weight,
):
    count = lax.axis_size("ep")
    own_rows, width = tokens.shape
    seqs, heads, size, _ = state.shape
    total = 2 * count
    narrow, full = jnp.bfloat16, jnp.float32
    turned = [
        w.transpose(1, 2, 0).reshape(-1, width) for w in (w_query, w_key, w_value, w_zgate)
    ]
    wide = 4 * turned[0].shape[0]
    swapped, rates = comm_call(
        functools.partial(project_kernel, count),
        1,
        (
            jax.ShapeDtypeStruct((count, seqs, wide), narrow),
            jax.ShapeDtypeStruct((seqs, 2 * heads), full),
        ),
        [tokens, mix_gain.reshape(1, width)] + turned + [w_beta.T, w_decay.T],
        [
            VMEM((own_rows, width), narrow),
            VMEM((total, own_rows, width), narrow),
            VMEM((count, seqs, wide), narrow),
        ]
        + sems(copies_of(count, True))
        + sems(count),
    )
    x = swapped.astype(full).transpose(1, 0, 2)
    gated, new_state = delta(decay_rate, decay_bias, rates, x, head_gain, state)
    resid, moe_all = comm_call(
        functools.partial(mix_kernel, count),
        2,
        (
            jax.ShapeDtypeStruct((own_rows, width), full),
            jax.ShapeDtypeStruct((total, own_rows, width), narrow),
        ),
        [gated, w_out, tokens, moe_gain.reshape(1, width)],
        [
            VMEM((count, seqs, heads * size), narrow),
            VMEM((total, own_rows, w_out.shape[1]), narrow),
            VMEM((total, own_rows, w_out.shape[1]), narrow),
            VMEM((own_rows, width), narrow),
        ]
        + sems(copies_of(count, False))
        + sems(total)
        + sems(copies_of(count, True)),
    )
    depth, side = grid_of(count)
    copies = count + (side - 1) * side * depth + (side - 1) * depth + depth - 1
    buf = lambda n: VMEM((n, own_rows, width), narrow)
    layer_out = comm_call(
        functools.partial(moe_kernel, count),
        3,
        jax.ShapeDtypeStruct((own_rows, width), narrow),
        [
            moe_all,
            resid,
            dense_mix.astype(full).reshape(1, width),
            dense_gate,
            dense_up,
            dense_down,
            expert_gate[0],
            expert_up[0],
            expert_down[0],
            expert_ids.T,
            route_weight.T,
        ],
        [buf(total)]
        + [buf(count)] * 3
        + [buf(side * depth)] * 2
        + [buf(depth)] * 2
        + sems(copies),
    )
    return (layer_out, new_state)


def solution(mesh):
    placed = (
        P(("ep", "tp"), None),
        P(),
        P(None, "tp", "ep"),
        P(None, "tp", "ep"),
        P(None, "tp", "ep"),
        P(None, "tp", "ep"),
        P(None, "tp"),
        P(None, "tp"),
        P("tp"),
        P("tp"),
        P(),
        P("ep", "tp", None, None),
        P("tp", "ep"),
        P(),
        P(),
        P(None, ("ep", "tp")),
        P(None, ("ep", "tp")),
        P(("ep", "tp"), None),
        P("ep", None, "tp"),
        P("ep", None, "tp"),
        P("ep", "tp", None),
        P(),
        P(),
    )
    return jax.shard_map(
        body,
        mesh=mesh,
        in_specs=placed,
        out_specs=(P(("ep", "tp"), None), P("ep", "tp", None, None)),
        check_vma=False,
    )
```
